32 devices in a mesh: ep: 8 (over z, x), tp: 4 (over y, core).
Axes of the slice: x: 2, y: 2, z: 4, core: 2. Of those that a mesh axis runs over, the one named last changes fastest.
Arguments:
- tokens: bfloat16 [2048, 2048], P('ep'), may hold values from -6 to 6
- norm_gain: float32 [2048], replicated, may hold values from 0.1 to 1.9
- expert_ids: int32 [2048, 4], P('ep'), may hold values from 0 to 7, all different within a row; in each aligned block of 256 rows (0 to 255, 256 to 511, ...) at most 256 rows name the same one
- route_weights: float32 [2048, 4], P('ep'), may hold values from 0.05 to 1
- gate_weight: bfloat16 [8, 2048, 2048], P('ep', None, 'tp'), as said below
- up_weight: bfloat16 [8, 2048, 2048], P('ep', None, 'tp'), as said below
- down_weight: bfloat16 [8, 2048, 2048], P('ep', 'tp'), may hold values from -0.125 to 0.125
Outputs:
- mixed: bfloat16 [2048, 2048], P('ep', 'tp')
The draws below stay inside these ranges and needn't reach their ends.
Inputs may be any that keep to these rules, and one draw needn't show every extreme that they name: `expert_ids`: each row names 4 different experts. In the rows of one device no expert is named by more than 256 rows, and in every draw some expert is named by exactly 256 rows of some device. `gate_weight`: independent entries of mean zero, drawn for each expert separately. `up_weight`: independent entries of mean zero, drawn for each expert separately.
All inputs are finite; a program needn't handle non-finite values.
Results may differ from the reference program's by a relative error of at most 0.014.
Values may be sent and summed in bfloat16 or wider, within the bound.
A program may use at most 128 MiB of HBM per device.

```python
import math
import jax
import jax.numpy as jnp
import numpy as np
from jax import lax

D = 2048
FF = 2048
TOP = 4
TOK_DEV = 256
EXPERTS = 8
CAP = 256
TOKENS = 2048
N_TP = 4


def draw_gate_weight(key, part):
    factor = 1.0
    values = jax.random.normal(jax.random.fold_in(key, 11), (EXPERTS, D, FF), jnp.float32)
    return (values * (factor / D ** 0.5)).astype(jnp.bfloat16)


def draw_up_weight(key, part):
    factor = 1.0
    values = jax.random.normal(jax.random.fold_in(key, 23), (EXPERTS, D, FF), jnp.float32)
    return (values * (factor / D ** 0.5)).astype(jnp.bfloat16)


def levels(stream_key, shape, split, smallest, largest):
    gain, own = 1.0, jax.random.fold_in(stream_key, 6)
    for dim, blocks in split:
        draws = jnp.exp(jax.random.uniform(jax.random.fold_in(own, dim), (blocks,), jnp.float32, smallest / len(split), largest / len(split)))
        gain = gain * jnp.repeat(draws, shape[dim] // blocks).reshape([-1 if axis == dim else 1 for axis in range(len(shape))])
    return gain


def deal_out(own_key, own, number, rows, count, top, most, lean):
    sequence = jax.random.permutation(own_key, count)
    heavy_load, ordinary = portions_of(count, rows * top, most, lean, True), portions_of(count, rows * top, most, lean, False)
    places = jnp.arange(count)

    def named(lengths, rotation):
        used = int((lengths > 0).sum())
        fixed = max(1, used // 4)
        moved = fixed + (places - fixed + rotation * (used - fixed)) % max(1, count - fixed)
        return jnp.zeros((count,), jnp.int32).at[sequence[jnp.where(places < fixed, places, moved)]].set(jnp.asarray(lengths, jnp.int32))

    lengths = jnp.where(number % 4 == 0, named(heavy_load, number // 4), named(ordinary, number - number // 4 - 1))
    mixed = jax.random.permutation(jax.random.fold_in(own, 3), count)
    source_of, sink = mixed[0:count // 2 * 2:2], mixed[1:count // 2 * 2:2]
    slack = jnp.minimum(lengths[source_of] - 1, most - lengths[sink]) // 2
    slack = jnp.where((source_of == sequence[0]) | (sink == sequence[0]) | (lengths[sink] == 0), 0, jnp.maximum(slack, 0))
    moved = jax.random.randint(jax.random.fold_in(own, 4), (count // 2,), 0, 1 << 20) % (slack + 1)
    lengths = lengths.at[source_of].add(-moved).at[sink].add(moved)
    labels = jnp.searchsorted(jnp.cumsum(lengths), jnp.arange(rows * top), side="right").astype(jnp.int32)
    listing = labels.reshape(top, rows).T
    listing = listing[jax.random.permutation(jax.random.fold_in(own, 1), rows)]
    rotation = jax.random.randint(jax.random.fold_in(own, 2), (rows, 1), 0, top)
    return jnp.take_along_axis(listing, (jnp.arange(top)[None, :] + rotation) % top, axis=1)


def portions_of(number_of, total, reach, slope, full):
    portions = [(1 << 20) // math.isqrt(standing ** slope) + 1 for standing in range(1, number_of + 1)]
    largest = reach if full else min(reach, max(-(-total // number_of), total * portions[0] // sum(portions)))
    least = 1 if total - largest >= number_of - 1 else 0
    holding, rest = [largest] + [least] * (number_of - 1), total - largest - least * (number_of - 1)
    while rest > 0:
        movable = [i for i in range(1, number_of) if holding[i] < largest] or [i for i in range(1, number_of) if holding[i] < reach]
        pool, remaining = sum([portions[i] for i in movable]), rest
        for i in movable:
            extra = min(reach - holding[i], max(1, remaining * portions[i] // pool), rest)
            holding[i] = holding[i] + extra
            rest = rest - extra
    return np.array(holding)


def scatter_about(stream_key, dims, scale, reach, shards=(), held_as=jnp.bfloat16):
    values = scale * jax.random.normal(stream_key, dims, jnp.float32)
    if shards:
        values = values * levels(stream_key, dims, shards, -0.22, 0.18)
    return jnp.clip(values, -reach, reach).astype(held_as)


def setup_inputs(seed: int = 0) -> dict:
    key_of = jax.random.split(jax.random.key(seed), 8)
    tokens = scatter_about(key_of[0], (TOKENS, D), 1.0, 6.0, ((0, 8),))
    norm_gain = jnp.clip(1.0 + 0.18 * jax.random.normal(key_of[1], (D,), jnp.float32), 0.1, 1.9)
    expert_ids_keys = jax.random.split(jax.random.fold_in(key_of[2], 1), TOKENS // TOK_DEV)
    expert_ids_turns = jax.random.permutation(jax.random.fold_in(key_of[2], 3), TOKENS // TOK_DEV)
    expert_ids = jax.vmap(lambda own, number: deal_out(jax.random.fold_in(key_of[2], 2), own, number, TOK_DEV, EXPERTS, TOP, CAP, 2))(expert_ids_keys, expert_ids_turns).reshape((TOKENS, TOP))
    route_weights = jnp.clip(0.05 + 0.95 * jax.random.uniform(key_of[3], (TOKENS, TOP), jnp.float32) ** levels(key_of[3], (TOKENS, TOP), ((0, 8),), -0.2, 0.2), 0.05, 1.0)
    gate_weight = draw_gate_weight(jax.random.fold_in(key_of[7], 71), 0)
    up_weight = draw_up_weight(jax.random.fold_in(key_of[7], 71), 0)
    down_weight = scatter_about(key_of[6], (EXPERTS, FF, D), FF ** -0.5, 0.125, ((0, 8), (1, 4)))
    return dict(tokens=tokens, norm_gain=norm_gain, expert_ids=expert_ids, route_weights=route_weights, gate_weight=gate_weight, up_weight=up_weight, down_weight=down_weight)


def reference(tokens, norm_gain, expert_ids, route_weights, gate_weight, up_weight, down_weight):
    values = tokens.astype(jnp.float32)
    scale = lax.rsqrt(lax.optimization_barrier(jnp.mean(values * values, axis=1, keepdims=True)) + 1e-06)
    normed = (values * scale * norm_gain[None, :]).astype(jnp.bfloat16)
    blocks = TOKENS // TOK_DEV
    pairs_dev = TOK_DEV * TOP
    flat = expert_ids.reshape(blocks, pairs_dev)
    onehot = (flat[:, :, None] == jnp.arange(EXPERTS, dtype=jnp.int32)[None, None, :]).astype(jnp.int32)
    before = jnp.cumsum(onehot, axis=1) - onehot
    slot = lax.optimization_barrier(jnp.sum(before * onehot, axis=2))
    source = jnp.arange(blocks, dtype=jnp.int32)[:, None]
    position = (slot + source * CAP).reshape(-1).astype(jnp.int32)
    pair_tok = (source * TOK_DEV + jnp.arange(pairs_dev, dtype=jnp.int32)[None, :] // TOP).reshape(-1).astype(jnp.int32)
    expert_flat = flat.reshape(-1).astype(jnp.int32)
    rows = blocks * CAP
    tok_table = jnp.zeros((EXPERTS, rows), jnp.int32).at[expert_flat, position].set(pair_tok)
    weight_table = jnp.zeros((EXPERTS, rows), jnp.float32).at[expert_flat, position].set(route_weights.reshape(-1))

    def one_expert(total, index):
        chosen = normed[tok_table[index]]
        gate = jnp.dot(chosen, gate_weight[index], preferred_element_type=jnp.float32)
        upper = jnp.dot(chosen, up_weight[index], preferred_element_type=jnp.float32)
        gate = jnp.minimum(gate, 7.0)
        upper = jnp.clip(upper, -7.0, 7.0)
        hidden = ((upper + 1.0) * (gate * jax.nn.sigmoid(1.702 * gate))).astype(jnp.bfloat16)
        blocked = hidden.reshape(rows, N_TP, FF // N_TP).astype(jnp.float32)
        down_blocks = down_weight[index].reshape(N_TP, FF // N_TP, D).astype(jnp.float32)
        partial_value = jnp.einsum('rpf,pfd->rpd', blocked, down_blocks).astype(jnp.bfloat16)
        expert_out = lax.optimization_barrier(jnp.sum(partial_value.astype(jnp.float32), axis=1)).astype(jnp.bfloat16)
        total = total.at[tok_table[index]].add(weight_table[index][:, None] * expert_out.astype(jnp.float32))
        return (total, None)
    start = jnp.zeros((TOKENS, D), jnp.float32)
    total, unused = lax.scan(one_expert, start, jnp.arange(EXPERTS, dtype=jnp.int32))
    return total.astype(jnp.bfloat16)
```

```python
import jax
import jax.numpy as jnp
from jax import lax
from jax.sharding import PartitionSpec as P


def normalise(tokens, norm_gain):
    values = tokens.astype(jnp.float32)
    scale = lax.rsqrt(jnp.mean(values * values, axis=1, keepdims=True) + 1e-06)
    return (values * scale * norm_gain[None, :]).astype(jnp.bfloat16)


def activate(gate, upper):
    gate = jnp.minimum(gate, 7.0)
    upper = jnp.clip(upper, -7.0, 7.0)
    return (upper + 1.0) * (gate * jax.nn.sigmoid(1.702 * gate))


def routed(tokens, norm_gain, expert_ids, route_weights, gate_weight, up_weight, down_weight):
    tok_dev, width = tokens.shape
    top = expert_ids.shape[1]
    n_ep = lax.axis_size("ep")
    n_tp = lax.axis_size("tp")
    exp_dev = gate_weight.shape[0]
    experts = exp_dev * n_ep
    capacity = 2 * tok_dev * top // experts
    quarter = width // n_tp
    normed = normalise(tokens, norm_gain)
    flat = expert_ids.reshape(-1)
    count = flat.shape[0]
    onehot = (flat[:, None] == jnp.arange(experts, dtype=jnp.int32)[None, :]).astype(jnp.int32)
    before = jnp.cumsum(onehot, axis=0) - onehot
    slot = jnp.sum(before * onehot, axis=1)
    position = flat * capacity + slot
    source_tok = jnp.arange(count, dtype=jnp.int32) // top
    buffer_tok = jnp.zeros((experts * capacity,), jnp.int32).at[position].set(source_tok)
    buffer_live = jnp.zeros((experts * capacity,), jnp.int32).at[position].set(1)
    columns = lax.dynamic_slice_in_dim(normed, lax.axis_index("tp") * quarter, quarter, 1)
    outgoing = jnp.where(buffer_live[:, None] > 0, columns[buffer_tok], jnp.zeros((), jnp.bfloat16))
    outgoing = outgoing.reshape(n_ep, exp_dev, capacity, quarter)
    received = lax.all_gather(
        lax.all_to_all(outgoing, "ep", split_axis=0, concat_axis=0, tiled=True),
        "tp",
        axis=3,
        tiled=True,
    )
    gate = jnp.einsum("sxcd,xdf->sxcf", received, gate_weight, preferred_element_type=jnp.float32)
    upper = jnp.einsum("sxcd,xdf->sxcf", received, up_weight, preferred_element_type=jnp.float32)
    hidden = activate(gate, upper).astype(jnp.bfloat16)
    partial_value = jnp.einsum(
        "sxcf,xfd->sxcd", hidden, down_weight, preferred_element_type=jnp.float32
    )
    rounded = partial_value.astype(jnp.bfloat16)
    summed = lax.psum_scatter(rounded, "tp", scatter_dimension=3, tiled=True)
    returned = lax.all_to_all(summed, "ep", split_axis=0, concat_axis=0, tiled=True)
    returned = returned.reshape(experts * capacity, quarter)
    picked = returned[position].reshape(tok_dev, top, quarter)
    mixed = jnp.sum(route_weights[:, :, None] * picked.astype(jnp.float32), axis=1)
    return mixed.astype(jnp.bfloat16)


def dense(tokens, norm_gain, expert_ids, route_weights, gate_weight, up_weight, down_weight):
    tok_dev, width = tokens.shape
    n_ep = lax.axis_size("ep")
    n_tp = lax.axis_size("tp")
    quarter = width // n_tp
    mine = lax.axis_index("ep")
    normed = normalise(tokens, norm_gain)
    columns = lax.dynamic_slice_in_dim(normed, lax.axis_index("tp") * quarter, quarter, 1)
    onehot = expert_ids[:, :, None] == jnp.arange(n_ep, dtype=jnp.int32)[None, None, :]
    table = jnp.sum(jnp.where(onehot, route_weights[:, :, None], 0.0), axis=1)
    weights = lax.all_to_all(table.T, "ep", split_axis=0, concat_axis=0, tiled=True)
    every = lax.all_gather(columns, ("ep", "tp"), axis=0, tiled=False)
    every = every.reshape(n_ep, n_tp, tok_dev, quarter)
    gate_w = gate_weight.reshape(n_tp, quarter, -1)
    up_w = up_weight.reshape(n_tp, quarter, -1)
    gate = jnp.einsum("epcd,pdf->ecf", every, gate_w, preferred_element_type=jnp.float32)
    upper = jnp.einsum("epcd,pdf->ecf", every, up_w, preferred_element_type=jnp.float32)
    hidden = activate(gate, upper).astype(jnp.bfloat16)
    down_w = down_weight[0].reshape(-1, n_tp, quarter)
    out = jnp.einsum("ecf,fpd->epcd", hidden, down_w, preferred_element_type=jnp.float32)
    out = jnp.where(weights[:, None, :, None] > 0, weights[:, None, :, None] * out, 0.0)
    out = out.astype(jnp.bfloat16).reshape(n_ep * n_tp, tok_dev, quarter)
    return lax.psum_scatter(out, ("ep", "tp"), scatter_dimension=0, tiled=False)


def per_device(tokens, norm_gain, expert_ids, route_weights, gate_weight, up_weight, down_weight):
    tok_dev, top = expert_ids.shape
    experts = gate_weight.shape[0] * lax.axis_size("ep")
    whole = gate_weight.shape[0] == 1 and 2 * tok_dev * top // experts >= tok_dev
    form = dense if whole else routed
    return form(
        tokens, norm_gain, expert_ids, route_weights, gate_weight, up_weight, down_weight
    )


def solution(mesh):
    in_specs = (
        P("ep", None),
        P(),
        P("ep", None),
        P("ep", None),
        P("ep", None, "tp"),
        P("ep", None, "tp"),
        P("ep", "tp", None),
    )
    return jax.shard_map(
        per_device, mesh=mesh, in_specs=in_specs, out_specs=P("ep", "tp"), check_vma=False
    )
```

```python
import functools

import jax
import jax.numpy as jnp
from jax import lax
from jax.experimental import pallas as pl
from jax.experimental.pallas import tpu as pltpu
from jax.sharding import PartitionSpec as P


MESH = pl.DeviceIdType.MESH


def normalise(tokens, norm_gain):
    values = tokens.astype(jnp.float32)
    scale = lax.rsqrt(jnp.mean(values * values, axis=1, keepdims=True) + 1e-06)
    return (values * scale * norm_gain[None, :]).astype(jnp.bfloat16)


def activate(gate, upper):
    gate = jnp.minimum(gate, 7.0)
    upper = jnp.clip(upper, -7.0, 7.0)
    return (upper + 1.0) * (gate * jax.nn.sigmoid(1.702 * gate))


def routed(tokens, norm_gain, expert_ids, route_weights, gate_weight, up_weight, down_weight):
    tok_dev, width = tokens.shape
    top = expert_ids.shape[1]
    n_ep = lax.axis_size("ep")
    n_tp = lax.axis_size("tp")
    exp_dev = gate_weight.shape[0]
    experts = exp_dev * n_ep
    capacity = 2 * tok_dev * top // experts
    quarter = width // n_tp
    normed = normalise(tokens, norm_gain)
    flat = expert_ids.reshape(-1)
    count = flat.shape[0]
    onehot = (flat[:, None] == jnp.arange(experts, dtype=jnp.int32)[None, :]).astype(jnp.int32)
    before = jnp.cumsum(onehot, axis=0) - onehot
    slot = jnp.sum(before * onehot, axis=1)
    position = flat * capacity + slot
    source_tok = jnp.arange(count, dtype=jnp.int32) // top
    buffer_tok = jnp.zeros((experts * capacity,), jnp.int32).at[position].set(source_tok)
    buffer_live = jnp.zeros((experts * capacity,), jnp.int32).at[position].set(1)
    columns = lax.dynamic_slice_in_dim(normed, lax.axis_index("tp") * quarter, quarter, 1)
    outgoing = jnp.where(buffer_live[:, None] > 0, columns[buffer_tok], jnp.zeros((), jnp.bfloat16))
    outgoing = outgoing.reshape(n_ep, exp_dev, capacity, quarter)
    received = lax.all_gather(
        lax.all_to_all(outgoing, "ep", split_axis=0, concat_axis=0, tiled=True),
        "tp",
        axis=3,
        tiled=True,
    )
    gate = jnp.einsum("sxcd,xdf->sxcf", received, gate_weight, preferred_element_type=jnp.float32)
    upper = jnp.einsum("sxcd,xdf->sxcf", received, up_weight, preferred_element_type=jnp.float32)
    hidden = activate(gate, upper).astype(jnp.bfloat16)
    partial_value = jnp.einsum(
        "sxcf,xfd->sxcd", hidden, down_weight, preferred_element_type=jnp.float32
    )
    rounded = partial_value.astype(jnp.bfloat16)
    summed = lax.psum_scatter(rounded, "tp", scatter_dimension=3, tiled=True)
    returned = lax.all_to_all(summed, "ep", split_axis=0, concat_axis=0, tiled=True)
    returned = returned.reshape(experts * capacity, quarter)
    picked = returned[position].reshape(tok_dev, top, quarter)
    mixed = jnp.sum(route_weights[:, :, None] * picked.astype(jnp.float32), axis=1)
    return mixed.astype(jnp.bfloat16)


def kernel(
    n_ep, tokens_ref, gain_ref, route_ref, gate_hbm, up_hbm, down_hbm, out_ref,
    gath, gate_w, up_w, down_w, hidden, part, dbuf, ya, xa, xb, yb, own, rup, rdn,
    w_sem, sz, rz, sx, rx, sy, ry, sd, rd,
    s_d, r_d, s_ya, r_ya, s_xb, r_xb, s_xa, r_xa, s_yb, r_yb, s_z, r_z,
):
    ep, tp = lax.axis_index("ep"), lax.axis_index("tp")
    z, x, y, c = ep // 2, ep % 2, tp // 2, tp % 2
    nz = n_ep // 2
    width = tokens_ref.shape[1]
    quarter = width // 4
    eighth = quarter // 2
    common = width // 8
    special = (width - 2 * common) // 4
    above = {"ep": lax.rem(ep + 2, n_ep), "tp": tp}
    below = {"ep": lax.rem(ep + n_ep - 2, n_ep), "tp": tp}
    xdev = {"ep": 2 * z + 1 - x, "tp": tp}
    ydev = {"ep": ep, "tp": 2 * (1 - y) + c}
    ddev = {"ep": ep, "tp": 2 * y + 1 - c}

    weight_copies = [
        pltpu.make_async_copy(gate_hbm.at[0], gate_w, w_sem.at[0]),
        pltpu.make_async_copy(up_hbm.at[0], up_w, w_sem.at[1]),
        pltpu.make_async_copy(down_hbm.at[0], down_w, w_sem.at[2]),
    ]
    for item in weight_copies:
        item.start()

    barrier = pltpu.get_barrier_semaphore()

    def greet(device):
        pl.semaphore_signal(barrier, inc=1, device_id=device, device_id_type=MESH)

    for device in (xdev, ydev, ddev):
        greet(device)

    @pl.when(z > 0)
    def _():
        greet(below)

    @pl.when(z < nz - 1)
    def _():
        greet(above)

    tile = 32

    def norm_step(i, carry):
        rows = pl.ds(pl.multiple_of(i * tile, tile), tile)
        values = tokens_ref[rows, :].astype(jnp.float32)
        scale = lax.rsqrt(jnp.mean(values * values, axis=1, keepdims=True) + 1e-06)
        gath[ep, rows, :] = (values * scale * gain_ref[...]).astype(jnp.bfloat16)
        return carry

    lax.fori_loop(0, tokens_ref.shape[0] // tile, norm_step, 0)
    greeted = 3 + jnp.where(z > 0, 1, 0) + jnp.where(z < nz - 1, 1, 0)
    pl.semaphore_wait(barrier, greeted)

    def cols(k, yy, cc):
        if k == 0:
            return pl.ds(pl.multiple_of(cc * common, 128), common)
        return pl.ds(pl.multiple_of(2 * common + (2 * yy + cc) * special, 128), special)

    def move(block, k, yy, cc, device, send, recv):
        ref = gath.at[block, :, cols(k, yy, cc)]
        return pltpu.make_async_remote_copy(
            src_ref=ref, dst_ref=ref, send_sem=send, recv_sem=recv,
            device_id=device, device_id_type=MESH,
        )

    def go_z(block, k, direction):
        device = above if direction == 0 else below
        return move(block, k, y, c, device, sz.at[direction, k, block], rz.at[k, block])

    def go_x(block, k):
        return move(block, k, y, c, xdev, sx.at[k, block], rx.at[k, block])

    def go_y(block, yy):
        return move(block, 1, yy, c, ydev, sy.at[block], ry.at[block])

    def go_d(block, kind, cc):
        k, yy = (0, y) if kind == 0 else (1, y if kind == 1 else 1 - y)
        return move(block, k, yy, cc, ddev, sd.at[kind, block], rd.at[kind, block])

    for k in (0, 1):
        @pl.when(z < nz - 1)
        def _():
            go_z(ep, k, 0).start()

        @pl.when(z > 0)
        def _():
            go_z(ep, k, 1).start()

        go_x(ep, k).start()

    def from_z(block, direction):
        for k in (1, 0):
            go_z(block, k, direction).wait_recv()

            @pl.when(z < nz - 1 if direction == 0 else z > 0)
            def _():
                go_z(block, k, direction).start()

            go_x(block, k).start()
            if k == 1:
                go_y(block, y).start()
            go_d(block, k, c).start()

    def from_x(block):
        for k in (1, 0):
            go_x(block, k).wait_recv()
            if k == 1:
                go_y(block, y).start()
            go_d(block, k, c).start()

    def from_y(block):
        go_y(block, 1 - y).wait_recv()
        go_d(block, 2, c).start()

    def at_distance(s, action):
        @pl.when(z - s >= 0)
        def _():
            action(z - s, 0)

        @pl.when(z + s <= nz - 1)
        def _():
            action(z + s, 1)

    for s in range(1, nz):
        at_distance(s, lambda row, way: from_z(2 * row + x, way))
        if s == 1:
            from_x(2 * z + 1 - x)
        else:
            at_distance(s - 1, lambda row, way: from_x(2 * row + 1 - x))
    at_distance(nz - 1, lambda row, way: from_x(2 * row + 1 - x))

    from_y(2 * z + 1 - x)
    for s in range(1, nz):
        at_distance(s, lambda row, way: from_y(2 * row + x))
        at_distance(s, lambda row, way: from_y(2 * row + 1 - x))

    def others(action):
        action(2 * z + 1 - x)
        for s in range(1, nz):
            at_distance(s, lambda row, way: action(2 * row + x))
            at_distance(s, lambda row, way: action(2 * row + 1 - x))

    def arrived(block):
        for kind in (0, 1, 2):
            go_d(block, kind, 1 - c).wait_recv()

    others(arrived)
    for item in weight_copies:
        item.wait()

    def span(start, size):
        return pl.ds(pl.multiple_of(start, 128), size)

    def send(src, dst, send_sem, recv_sem, device):
        return pltpu.make_async_remote_copy(
            src_ref=src, dst_ref=dst, send_sem=send_sem, recv_sem=recv_sem,
            device_id=device, device_id_type=MESH,
        )

    def d_copy(r, yq, cc):
        return send(
            part.at[pl.ds(2 * r, 2), :, span((2 * yq + cc) * quarter, quarter)],
            dbuf.at[pl.ds(2 * r, 2), :, span(yq * quarter, quarter)],
            s_d.at[r, yq], r_d.at[r, yq], ddev,
        )

    def ya_copy(r):
        return send(
            dbuf.at[pl.ds(2 * r, 2), :, span((1 - y) * quarter, eighth)],
            ya.at[pl.ds(2 * r, 2)], s_ya.at[r], r_ya.at[r], ydev,
        )

    def xb_copy(r, yq):
        return send(
            dbuf.at[2 * r + 1 - x, :, span(yq * quarter + eighth, eighth)],
            xb.at[r, :, span(yq * eighth, eighth)], s_xb.at[r, yq], r_xb.at[r, yq], xdev,
        )

    def xa_copy(r):
        return send(ya.at[2 * r + 1 - x], xa.at[r], s_xa.at[r], r_xa.at[r], xdev)

    def yb_copy(r):
        return send(
            xb.at[r, :, span((1 - y) * eighth, eighth)],
            yb.at[r], s_yb.at[r], r_yb.at[r], ydev,
        )

    def up_copy(r):
        return send(own.at[r], rup.at[r], s_z.at[0, r], r_z.at[0, r], above)

    def dn_copy(r):
        return send(own.at[r], rdn.at[r], s_z.at[1, r], r_z.at[1, r], below)

    def add(a, b):
        return (a.astype(jnp.float32) + b.astype(jnp.float32)).astype(jnp.bfloat16)

    rows = tokens_ref.shape[0]
    ff = gate_w.shape[1]
    fstep = min(256, ff)

    def compute(r):
        lhs_of = lambda: gath[pl.ds(2 * r, 2)].reshape(2 * rows, width)
        route = route_ref[pl.ds(2 * r, 2)].reshape(2 * rows, 128)
        route = jnp.concatenate([route] * (fstep // 128), axis=1)

        def ff_step(j, carry):
            at = span(j * fstep, fstep)
            lhs = lhs_of()
            gate = jnp.dot(lhs, gate_w[:, at], preferred_element_type=jnp.float32)
            upper = jnp.dot(lhs, up_w[:, at], preferred_element_type=jnp.float32)
            value = activate(gate, upper)
            hidden[:, at] = jnp.where(route > 0, route * value, 0.0).astype(jnp.bfloat16)
            return carry

        lax.fori_loop(0, ff // fstep, ff_step, 0)

        def down_step(j, carry):
            yq = j % 2
            cc = jnp.where(j < 2, 1 - c, c)
            at = span((2 * yq + cc) * quarter, quarter)
            value = jnp.dot(hidden[...], down_w[:, at], preferred_element_type=jnp.float32)
            part[pl.ds(2 * r, 2), :, at] = value.astype(jnp.bfloat16).reshape(2, rows, quarter)

            @pl.when(j < 2)
            def _():
                d_copy(r, yq, 1 - c).start()

            return carry

        lax.fori_loop(0, 4, down_step, 0)

    def stage_a(r):
        for yq in (0, 1):
            d_copy(r, yq, 1 - c).wait_recv()
            mine = part[pl.ds(2 * r, 2), :, span((2 * yq + c) * quarter, quarter)]
            at = span(yq * quarter, quarter)
            dbuf[pl.ds(2 * r, 2), :, at] = add(mine, dbuf[pl.ds(2 * r, 2), :, at])
        ya_copy(r).start()
        for yq in (0, 1):
            xb_copy(r, yq).start()

    def stage_b(r):
        ya_copy(r).wait_recv()
        ya[pl.ds(2 * r, 2)] = add(
            dbuf[pl.ds(2 * r, 2), :, span(y * quarter, eighth)], ya[pl.ds(2 * r, 2)]
        )
        xa_copy(r).start()
        for yq in (0, 1):
            xb_copy(r, yq).wait_recv()
            at = span(yq * eighth, eighth)
            mine = dbuf[2 * r + x, :, span(yq * quarter + eighth, eighth)]
            xb[r, :, at] = add(mine, xb[r, :, at])
        yb_copy(r).start()

    def stage_c(r):
        xa_copy(r).wait_recv()
        own[r, :, 0:eighth] = add(ya[2 * r + x], xa[r])
        yb_copy(r).wait_recv()
        own[r, :, eighth:quarter] = add(xb[r, :, span(y * eighth, eighth)], yb[r])

    def stage_d(r):
        @pl.when((z > 0) & (z <= r))
        def _():
            up_copy(r).wait_recv()
            own[r] = add(own[r], rup[r])

        @pl.when((z < nz - 1) & (z >= r))
        def _():
            dn_copy(r).wait_recv()
            own[r] = add(own[r], rdn[r])

        @pl.when(z < r)
        def _():
            up_copy(r).start()

        @pl.when(z > r)
        def _():
            dn_copy(r).start()

        @pl.when(z == r)
        def _():
            out_ref[...] = own[r]

    def row_of(i):
        odd = i % 2
        return (1 - odd) * (nz - 1 - i // 2) + odd * (i // 2)

    def step(i, carry):
        @pl.when(i < nz)
        def _():
            compute(row_of(i))
            stage_a(row_of(i))

        @pl.when((i >= 1) & (i < nz + 1))
        def _():
            stage_b(row_of(i - 1))

        @pl.when((i >= 2) & (i < nz + 2))
        def _():
            stage_c(row_of(i - 2))
            stage_d(row_of(i - 2))

        return carry

    lax.fori_loop(0, nz + 2, step, 0)

    def sent(block, direction):
        for k in (0, 1):
            @pl.when(z < nz - 1 if direction == 0 else z > 0)
            def _():
                go_z(block, k, direction).wait_send()

            go_x(block, k).wait_send()

    for k in (0, 1):
        @pl.when(z < nz - 1)
        def _():
            go_z(ep, k, 0).wait_send()

        @pl.when(z > 0)
        def _():
            go_z(ep, k, 1).wait_send()

        go_x(ep, k).wait_send()
    for s in range(1, nz):
        at_distance(s, lambda row, way: sent(2 * row + x, way))

    def passed(block):
        go_y(block, y).wait_send()
        for kind in (0, 1, 2):
            go_d(block, kind, c).wait_send()

    others(passed)

    def finish(r, carry):
        for yq in (0, 1):
            d_copy(r, yq, 1 - c).wait_send()
            xb_copy(r, yq).wait_send()
        ya_copy(r).wait_send()
        xa_copy(r).wait_send()
        yb_copy(r).wait_send()

        @pl.when(z < r)
        def _():
            up_copy(r).wait_send()

        @pl.when(z > r)
        def _():
            dn_copy(r).wait_send()

        return carry

    lax.fori_loop(0, nz, finish, 0)


def dense(tokens, norm_gain, expert_ids, route_weights, gate_weight, up_weight, down_weight):
    rows, width = tokens.shape
    n_ep = lax.axis_size("ep")
    nz = n_ep // 2
    ff = gate_weight.shape[2]
    quarter = width // lax.axis_size("tp")
    eighth = quarter // 2
    onehot = expert_ids[:, :, None] == jnp.arange(n_ep, dtype=jnp.int32)[None, None, :]
    table = jnp.sum(jnp.where(onehot, route_weights[:, :, None], 0.0), axis=1)
    weights = lax.all_to_all(table.T, "ep", split_axis=0, concat_axis=0, tiled=True)
    weights = jnp.broadcast_to(weights[:, :, None], (n_ep, rows, 128))
    vmem = pl.BlockSpec(memory_space=pltpu.VMEM)
    hbm = pl.BlockSpec(memory_space=pl.ANY)
    bf16 = jnp.bfloat16
    dma = pltpu.SemaphoreType.DMA
    return pl.pallas_call(
        functools.partial(kernel, n_ep),
        out_shape=jax.ShapeDtypeStruct((rows, quarter), bf16),
        in_specs=[vmem, vmem, vmem, hbm, hbm, hbm],
        out_specs=vmem,
        scratch_shapes=[
            pltpu.VMEM((n_ep, rows, width), bf16),
            pltpu.VMEM((width, ff), bf16),
            pltpu.VMEM((width, ff), bf16),
            pltpu.VMEM((ff, width), bf16),
            pltpu.VMEM((2 * rows, ff), bf16),
            pltpu.VMEM((n_ep, rows, width), bf16),
            pltpu.VMEM((n_ep, rows, 2 * quarter), bf16),
            pltpu.VMEM((n_ep, rows, eighth), bf16),
            pltpu.VMEM((nz, rows, eighth), bf16),
            pltpu.VMEM((nz, rows, 2 * eighth), bf16),
            pltpu.VMEM((nz, rows, eighth), bf16),
            pltpu.VMEM((nz, rows, quarter), bf16),
            pltpu.VMEM((nz, rows, quarter), bf16),
            pltpu.VMEM((nz, rows, quarter), bf16),
            dma((3,)),
            dma((2, 2, n_ep)), dma((2, n_ep)),
            dma((2, n_ep)), dma((2, n_ep)),
            dma((n_ep,)), dma((n_ep,)),
            dma((3, n_ep)), dma((3, n_ep)),
            dma((nz, 2)), dma((nz, 2)),
            dma((nz,)), dma((nz,)),
            dma((nz, 2)), dma((nz, 2)),
            dma((nz,)), dma((nz,)),
            dma((nz,)), dma((nz,)),
            dma((2, nz)), dma((2, nz)),
        ],
        compiler_params=pltpu.CompilerParams(
            collective_id=0, has_side_effects=True, vmem_limit_bytes=60 * 1024 * 1024
        ),
    )(tokens, norm_gain[None, :], weights, gate_weight, up_weight, down_weight)


def per_device(tokens, norm_gain, expert_ids, route_weights, gate_weight, up_weight, down_weight):
    tok_dev, top = expert_ids.shape
    experts = gate_weight.shape[0] * lax.axis_size("ep")
    whole = gate_weight.shape[0] == 1 and 2 * tok_dev * top // experts >= tok_dev
    whole = whole and lax.axis_size("tp") == 4 and lax.axis_size("ep") % 2 == 0
    form = dense if whole and tokens.shape[1] % 2048 == 0 else routed
    return form(
        tokens, norm_gain, expert_ids, route_weights, gate_weight, up_weight, down_weight
    )


def solution(mesh):
    in_specs = (
        P("ep", None),
        P(),
        P("ep", None),
        P("ep", None),
        P("ep", None, "tp"),
        P("ep", None, "tp"),
        P("ep", "tp", None),
    )
    return jax.shard_map(
        per_device, mesh=mesh, in_specs=in_specs, out_specs=P("ep", "tp"), check_vma=False
    )
```

```python
import functools

import jax
import jax.numpy as jnp
from jax import lax
from jax.experimental import pallas as pl
from jax.experimental.pallas import tpu as pltpu
from jax.sharding import PartitionSpec as P


MESH = pl.DeviceIdType.MESH


def normalise(tokens, norm_gain):
    values = tokens.astype(jnp.float32)
    scale = lax.rsqrt(jnp.mean(values * values, axis=1, keepdims=True) + 1e-06)
    return (values * scale * norm_gain[None, :]).astype(jnp.bfloat16)


def activate(gate, upper):
    gate = jnp.minimum(gate, 7.0)
    upper = jnp.clip(upper, -7.0, 7.0)
    return (upper + 1.0) * (gate * jax.nn.sigmoid(1.702 * gate))


def routed(tokens, norm_gain, expert_ids, route_weights, gate_weight, up_weight, down_weight):
    tok_dev, width = tokens.shape
    top = expert_ids.shape[1]
    n_ep = lax.axis_size("ep")
    n_tp = lax.axis_size("tp")
    exp_dev = gate_weight.shape[0]
    experts = exp_dev * n_ep
    capacity = 2 * tok_dev * top // experts
    quarter = width // n_tp
    normed = normalise(tokens, norm_gain)
    flat = expert_ids.reshape(-1)
    count = flat.shape[0]
    onehot = (flat[:, None] == jnp.arange(experts, dtype=jnp.int32)[None, :]).astype(jnp.int32)
    before = jnp.cumsum(onehot, axis=0) - onehot
    slot = jnp.sum(before * onehot, axis=1)
    position = flat * capacity + slot
    source_tok = jnp.arange(count, dtype=jnp.int32) // top
    buffer_tok = jnp.zeros((experts * capacity,), jnp.int32).at[position].set(source_tok)
    buffer_live = jnp.zeros((experts * capacity,), jnp.int32).at[position].set(1)
    columns = lax.dynamic_slice_in_dim(normed, lax.axis_index("tp") * quarter, quarter, 1)
    outgoing = jnp.where(buffer_live[:, None] > 0, columns[buffer_tok], jnp.zeros((), jnp.bfloat16))
    outgoing = outgoing.reshape(n_ep, exp_dev, capacity, quarter)
    received = lax.all_gather(
        lax.all_to_all(outgoing, "ep", split_axis=0, concat_axis=0, tiled=True),
        "tp",
        axis=3,
        tiled=True,
    )
    gate = jnp.einsum("sxcd,xdf->sxcf", received, gate_weight, preferred_element_type=jnp.float32)
    upper = jnp.einsum("sxcd,xdf->sxcf", received, up_weight, preferred_element_type=jnp.float32)
    hidden = activate(gate, upper).astype(jnp.bfloat16)
    partial_value = jnp.einsum(
        "sxcf,xfd->sxcd", hidden, down_weight, preferred_element_type=jnp.float32
    )
    rounded = partial_value.astype(jnp.bfloat16)
    summed = lax.psum_scatter(rounded, "tp", scatter_dimension=3, tiled=True)
    returned = lax.all_to_all(summed, "ep", split_axis=0, concat_axis=0, tiled=True)
    returned = returned.reshape(experts * capacity, quarter)
    picked = returned[position].reshape(tok_dev, top, quarter)
    mixed = jnp.sum(route_weights[:, :, None] * picked.astype(jnp.float32), axis=1)
    return mixed.astype(jnp.bfloat16)


def kernel(
    n_ep, tokens_ref, gain_ref, route_ref, gate_hbm, up_hbm, down_hbm, out_ref,
    gath, gtab, route_buf, gate_w, up_w, down_w, hidden, part, dbuf, ya, xa, xb, yb, own, rup, rdn,
    w_sem, sz, rz, sx, rx, sy, ry, sd, rd,
    s_d, r_d, s_ya, r_ya, s_xb, r_xb, s_xa, r_xa, s_yb, r_yb, s_z, r_z,
):
    ep, tp = lax.axis_index("ep"), lax.axis_index("tp")
    z, x, y, c = ep // 2, ep % 2, tp // 2, tp % 2
    nz = n_ep // 2
    width = tokens_ref.shape[1]
    quarter = width // 4
    eighth = quarter // 2
    common = width // 8
    special = (width - 2 * common) // 4
    above = {"ep": lax.rem(ep + 2, n_ep), "tp": tp}
    below = {"ep": lax.rem(ep + n_ep - 2, n_ep), "tp": tp}
    xdev = {"ep": 2 * z + 1 - x, "tp": tp}
    ydev = {"ep": ep, "tp": 2 * (1 - y) + c}
    ddev = {"ep": ep, "tp": 2 * y + 1 - c}

    weight_copies = [
        pltpu.make_async_copy(gate_hbm.at[0], gate_w, w_sem.at[0]),
        pltpu.make_async_copy(up_hbm.at[0], up_w, w_sem.at[1]),
        pltpu.make_async_copy(down_hbm.at[0], down_w, w_sem.at[2]),
    ]
    for item in weight_copies:
        item.start()

    barrier = pltpu.get_barrier_semaphore()

    def greet(device):
        pl.semaphore_signal(barrier, inc=1, device_id=device, device_id_type=MESH)

    for device in (xdev, ydev, ddev):
        greet(device)

    @pl.when(z > 0)
    def _():
        greet(below)

    @pl.when(z < nz - 1)
    def _():
        greet(above)

    tile = 32

    def norm_step(i, carry):
        rows = pl.ds(pl.multiple_of(i * tile, tile), tile)
        values = tokens_ref[rows, :].astype(jnp.float32)
        scale = lax.rsqrt(jnp.mean(values * values, axis=1, keepdims=True) + 1e-06)
        gath[ep, rows, :] = (values * scale * gain_ref[...]).astype(jnp.bfloat16)
        return carry

    lax.fori_loop(0, tokens_ref.shape[0] // tile, norm_step, 0)
    gtab[ep] = route_ref[...]
    greeted = 3 + jnp.where(z > 0, 1, 0) + jnp.where(z < nz - 1, 1, 0)
    pl.semaphore_wait(barrier, greeted)

    def cols(k, yy, cc):
        if k == 0:
            return pl.ds(pl.multiple_of(cc * common, 128), common)
        return pl.ds(pl.multiple_of(2 * common + (2 * yy + cc) * special, 128), special)

    def move(block, k, yy, cc, device, send, recv):
        ref = gtab.at[block] if k == 2 else gath.at[block, :, cols(k, yy, cc)]
        return pltpu.make_async_remote_copy(
            src_ref=ref, dst_ref=ref, send_sem=send, recv_sem=recv,
            device_id=device, device_id_type=MESH,
        )

    def go_z(block, k, direction):
        device = above if direction == 0 else below
        return move(block, k, y, c, device, sz.at[direction, k, block], rz.at[k, block])

    def go_x(block, k):
        return move(block, k, y, c, xdev, sx.at[k, block], rx.at[k, block])

    def go_y(block, yy):
        return move(block, 1, yy, c, ydev, sy.at[block], ry.at[block])

    def go_d(block, kind, cc):
        k, yy = (0, y) if kind == 0 else (1, y if kind == 1 else 1 - y)
        return move(block, k, yy, cc, ddev, sd.at[kind, block], rd.at[kind, block])

    for k in (1, 2, 0):
        @pl.when(z < nz - 1)
        def _():
            go_z(ep, k, 0).start()

        @pl.when(z > 0)
        def _():
            go_z(ep, k, 1).start()

        go_x(ep, k).start()

    def from_z(block, direction):
        for k in (1, 2, 0):
            go_z(block, k, direction).wait_recv()

            @pl.when(z < nz - 1 if direction == 0 else z > 0)
            def _():
                go_z(block, k, direction).start()

            go_x(block, k).start()
            if k == 1:
                go_y(block, y).start()
            if k < 2:
                go_d(block, k, c).start()

    def from_x(block):
        for k in (1, 2, 0):
            go_x(block, k).wait_recv()
            if k == 1:
                go_y(block, y).start()
            if k < 2:
                go_d(block, k, c).start()

    def from_y(block):
        go_y(block, 1 - y).wait_recv()
        go_d(block, 2, c).start()

    def at_distance(s, action):
        @pl.when(z - s >= 0)
        def _():
            action(z - s, 0)

        @pl.when(z + s <= nz - 1)
        def _():
            action(z + s, 1)

    for s in range(1, nz):
        at_distance(s, lambda row, way: from_z(2 * row + x, way))
        if s == 1:
            from_x(2 * z + 1 - x)
        else:
            at_distance(s - 1, lambda row, way: from_x(2 * row + 1 - x))
    at_distance(nz - 1, lambda row, way: from_x(2 * row + 1 - x))

    def others(action):
        action(2 * z + 1 - x)
        for s in range(1, nz):
            at_distance(s, lambda row, way: action(2 * row + x))
            at_distance(s, lambda row, way: action(2 * row + 1 - x))

    def arrived(block):
        for kind in (0, 1, 2):
            go_d(block, kind, 1 - c).wait_recv()

    def span(start, size):
        return pl.ds(pl.multiple_of(start, 128), size)

    def send(src, dst, send_sem, recv_sem, device):
        return pltpu.make_async_remote_copy(
            src_ref=src, dst_ref=dst, send_sem=send_sem, recv_sem=recv_sem,
            device_id=device, device_id_type=MESH,
        )

    def d_copy(r, yq, cc):
        return send(
            part.at[pl.ds(2 * r, 2), :, span((2 * yq + cc) * quarter, quarter)],
            dbuf.at[pl.ds(2 * r, 2), :, span(yq * quarter, quarter)],
            s_d.at[r, yq], r_d.at[r, yq], ddev,
        )

    def ya_copy(r):
        return send(
            dbuf.at[pl.ds(2 * r, 2), :, span((1 - y) * quarter, eighth)],
            ya.at[pl.ds(2 * r, 2)], s_ya.at[r], r_ya.at[r], ydev,
        )

    def xb_copy(r, yq):
        return send(
            dbuf.at[2 * r + 1 - x, :, span(yq * quarter + eighth, eighth)],
            xb.at[r, :, span(yq * eighth, eighth)], s_xb.at[r, yq], r_xb.at[r, yq], xdev,
        )

    def xa_copy(r):
        return send(ya.at[2 * r + 1 - x], xa.at[r], s_xa.at[r], r_xa.at[r], xdev)

    def yb_copy(r):
        return send(
            xb.at[r, :, span((1 - y) * eighth, eighth)],
            yb.at[r], s_yb.at[r], r_yb.at[r], ydev,
        )

    def up_copy(r):
        return send(own.at[r], rup.at[r], s_z.at[0, r], r_z.at[0, r], above)

    def dn_copy(r):
        return send(own.at[r], rdn.at[r], s_z.at[1, r], r_z.at[1, r], below)

    def add(a, b):
        return (a.astype(jnp.float32) + b.astype(jnp.float32)).astype(jnp.bfloat16)

    rows = tokens_ref.shape[0]
    ff = gate_w.shape[1]
    fstep = min(256, ff)

    def compute(r):
        lhs_of = lambda: gath[pl.ds(2 * r, 2)].reshape(2 * rows, width)
        for j in (0, 1):
            flipped = jnp.transpose(gtab[2 * r + j])
            lane = lax.broadcasted_iota(jnp.int32, flipped.shape, 1)
            column = jnp.sum(jnp.where(lane == ep, flipped, 0.0), axis=1, keepdims=True)
            route_buf[j * rows:(j + 1) * rows, :] = jnp.broadcast_to(column, (rows, 128))
        route = jnp.concatenate([route_buf[...]] * (fstep // 128), axis=1)

        def ff_step(j, carry):
            at = span(j * fstep, fstep)
            lhs = lhs_of()
            gate = jnp.dot(lhs, gate_w[:, at], preferred_element_type=jnp.float32)
            upper = jnp.dot(lhs, up_w[:, at], preferred_element_type=jnp.float32)
            value = activate(gate, upper)
            hidden[:, at] = jnp.where(route > 0, route * value, 0.0).astype(jnp.bfloat16)
            return carry

        lax.fori_loop(0, ff // fstep, ff_step, 0)

        def down_step(j, carry):
            yq = j % 2
            cc = jnp.where(j < 2, 1 - c, c)
            at = span((2 * yq + cc) * quarter, quarter)
            value = jnp.dot(hidden[...], down_w[:, at], preferred_element_type=jnp.float32)
            part[pl.ds(2 * r, 2), :, at] = value.astype(jnp.bfloat16).reshape(2, rows, quarter)

            @pl.when(j < 2)
            def _():
                d_copy(r, yq, 1 - c).start()

            return carry

        lax.fori_loop(0, 4, down_step, 0)

    def stage_a(r):
        for yq in (0, 1):
            d_copy(r, yq, 1 - c).wait_recv()
            mine = part[pl.ds(2 * r, 2), :, span((2 * yq + c) * quarter, quarter)]
            at = span(yq * quarter, quarter)
            dbuf[pl.ds(2 * r, 2), :, at] = add(mine, dbuf[pl.ds(2 * r, 2), :, at])
        ya_copy(r).start()
        for yq in (0, 1):
            xb_copy(r, yq).start()

    def stage_b(r):
        ya_copy(r).wait_recv()
        ya[pl.ds(2 * r, 2)] = add(
            dbuf[pl.ds(2 * r, 2), :, span(y * quarter, eighth)], ya[pl.ds(2 * r, 2)]
        )
        xa_copy(r).start()
        for yq in (0, 1):
            xb_copy(r, yq).wait_recv()
            at = span(yq * eighth, eighth)
            mine = dbuf[2 * r + x, :, span(yq * quarter + eighth, eighth)]
            xb[r, :, at] = add(mine, xb[r, :, at])
        yb_copy(r).start()

    def stage_c(r):
        xa_copy(r).wait_recv()
        own[r, :, 0:eighth] = add(ya[2 * r + x], xa[r])
        yb_copy(r).wait_recv()
        own[r, :, eighth:quarter] = add(xb[r, :, span(y * eighth, eighth)], yb[r])

    def stage_d(r):
        @pl.when((z > 0) & (z <= r))
        def _():
            up_copy(r).wait_recv()
            own[r] = add(own[r], rup[r])

        @pl.when((z < nz - 1) & (z >= r))
        def _():
            dn_copy(r).wait_recv()
            own[r] = add(own[r], rdn[r])

        @pl.when(z < r)
        def _():
            up_copy(r).start()

        @pl.when(z > r)
        def _():
            dn_copy(r).start()

        @pl.when(z == r)
        def _():
            out_ref[...] = own[r]

    last_first = [nz - 1 - i // 2 if i % 2 == 0 else i // 2 for i in range(nz)]
    order = [[k] + [r for r in last_first if r != k] for k in range(nz)]
    due = [[order[k].index(r) + 2 for r in range(nz)] for k in range(nz)]
    for r in range(nz):
        for k in range(1, r):
            due[k][r] = max(due[k][r], due[k - 1][r] + 1)
        for k in range(nz - 2, r, -1):
            due[k][r] = max(due[k][r], due[k + 1][r] + 1)
        for k in (r - 1, r + 1):
            if 0 <= k < nz:
                due[r][r] = max(due[r][r], due[k][r] + 1)
    steps = max(max(line) for line in due) + 1

    def row_of(i):
        row = z
        for k in range(nz):
            for j in range(1, nz):
                row = jnp.where((z == k) & (i == j), order[k][j], row)
        return row

    def step(i, carry):
        @pl.when(i == 1)
        def _():
            for s in range(1, nz):
                at_distance(s, lambda row, way: from_y(2 * row + x))
                at_distance(s, lambda row, way: from_y(2 * row + 1 - x))
            for s in range(1, nz):
                at_distance(s, lambda row, way: arrived(2 * row + x))
                at_distance(s, lambda row, way: arrived(2 * row + 1 - x))

        @pl.when(i < nz)
        def _():
            compute(row_of(i))
            stage_a(row_of(i))

        @pl.when((i >= 1) & (i < nz + 1))
        def _():
            stage_b(row_of(i - 1))

        @pl.when((i >= 2) & (i < nz + 2))
        def _():
            stage_c(row_of(i - 2))

        def chain(r, inner):
            when = 0
            for k in range(nz):
                for j in range(nz):
                    when = jnp.where((z == k) & (r == j), due[k][j], when)

            @pl.when(i == when)
            def _():
                stage_d(r)

            return inner

        lax.fori_loop(0, nz, chain, 0)
        return carry

    from_y(2 * z + 1 - x)
    arrived(2 * z + 1 - x)
    for item in weight_copies:
        item.wait()
    lax.fori_loop(0, steps, step, 0)

    def sent(block, direction):
        for k in (0, 1, 2):
            @pl.when(z < nz - 1 if direction == 0 else z > 0)
            def _():
                go_z(block, k, direction).wait_send()

            go_x(block, k).wait_send()

    for k in (0, 1, 2):
        @pl.when(z < nz - 1)
        def _():
            go_z(ep, k, 0).wait_send()

        @pl.when(z > 0)
        def _():
            go_z(ep, k, 1).wait_send()

        go_x(ep, k).wait_send()
    for s in range(1, nz):
        at_distance(s, lambda row, way: sent(2 * row + x, way))

    def passed(block):
        go_y(block, y).wait_send()
        for kind in (0, 1, 2):
            go_d(block, kind, c).wait_send()

    others(passed)

    def finish(r, carry):
        for yq in (0, 1):
            d_copy(r, yq, 1 - c).wait_send()
            xb_copy(r, yq).wait_send()
        ya_copy(r).wait_send()
        xa_copy(r).wait_send()
        yb_copy(r).wait_send()

        @pl.when(z < r)
        def _():
            up_copy(r).wait_send()

        @pl.when(z > r)
        def _():
            dn_copy(r).wait_send()

        return carry

    lax.fori_loop(0, nz, finish, 0)


def dense(tokens, norm_gain, expert_ids, route_weights, gate_weight, up_weight, down_weight):
    rows, width = tokens.shape
    n_ep = lax.axis_size("ep")
    nz = n_ep // 2
    ff = gate_weight.shape[2]
    quarter = width // lax.axis_size("tp")
    eighth = quarter // 2
    onehot = expert_ids[:, :, None] == jnp.arange(n_ep, dtype=jnp.int32)[None, None, :]
    table = jnp.sum(jnp.where(onehot, route_weights[:, :, None], 0.0), axis=1)
    vmem = pl.BlockSpec(memory_space=pltpu.VMEM)
    hbm = pl.BlockSpec(memory_space=pl.ANY)
    bf16 = jnp.bfloat16
    dma = pltpu.SemaphoreType.DMA
    return pl.pallas_call(
        functools.partial(kernel, n_ep),
        out_shape=jax.ShapeDtypeStruct((rows, quarter), bf16),
        in_specs=[vmem, vmem, vmem, hbm, hbm, hbm],
        out_specs=vmem,
        scratch_shapes=[
            pltpu.VMEM((n_ep, rows, width), bf16),
            pltpu.VMEM((n_ep, n_ep, rows), jnp.float32),
            pltpu.VMEM((2 * rows, 128), jnp.float32),
            pltpu.VMEM((width, ff), bf16),
            pltpu.VMEM((width, ff), bf16),
            pltpu.VMEM((ff, width), bf16),
            pltpu.VMEM((2 * rows, ff), bf16),
            pltpu.VMEM((n_ep, rows, width), bf16),
            pltpu.VMEM((n_ep, rows, 2 * quarter), bf16),
            pltpu.VMEM((n_ep, rows, eighth), bf16),
            pltpu.VMEM((nz, rows, eighth), bf16),
            pltpu.VMEM((nz, rows, 2 * eighth), bf16),
            pltpu.VMEM((nz, rows, eighth), bf16),
            pltpu.VMEM((nz, rows, quarter), bf16),
            pltpu.VMEM((nz, rows, quarter), bf16),
            pltpu.VMEM((nz, rows, quarter), bf16),
            dma((3,)),
            dma((2, 3, n_ep)), dma((3, n_ep)),
            dma((3, n_ep)), dma((3, n_ep)),
            dma((n_ep,)), dma((n_ep,)),
            dma((3, n_ep)), dma((3, n_ep)),
            dma((nz, 2)), dma((nz, 2)),
            dma((nz,)), dma((nz,)),
            dma((nz, 2)), dma((nz, 2)),
            dma((nz,)), dma((nz,)),
            dma((nz,)), dma((nz,)),
            dma((2, nz)), dma((2, nz)),
        ],
        compiler_params=pltpu.CompilerParams(
            collective_id=0, has_side_effects=True, vmem_limit_bytes=60 * 1024 * 1024
        ),
    )(tokens, norm_gain[None, :], table.T, gate_weight, up_weight, down_weight)


def per_device(tokens, norm_gain, expert_ids, route_weights, gate_weight, up_weight, down_weight):
    tok_dev, top = expert_ids.shape
    experts = gate_weight.shape[0] * lax.axis_size("ep")
    whole = gate_weight.shape[0] == 1 and 2 * tok_dev * top // experts >= tok_dev
    whole = whole and lax.axis_size("tp") == 4 and lax.axis_size("ep") % 2 == 0
    form = dense if whole and tokens.shape[1] % 2048 == 0 else routed
    return form(
        tokens, norm_gain, expert_ids, route_weights, gate_weight, up_weight, down_weight
    )


def solution(mesh):
    in_specs = (
        P("ep", None),
        P(),
        P("ep", None),
        P("ep", None),
        P("ep", None, "tp"),
        P("ep", None, "tp"),
        P("ep", "tp", None),
    )
    return jax.shard_map(
        per_device, mesh=mesh, in_specs=in_specs, out_specs=P("ep", "tp"), check_vma=False
    )
```

```python
import functools

import jax
import jax.numpy as jnp
from jax import lax
from jax.experimental import pallas as pl
from jax.experimental.pallas import tpu as pltpu
from jax.sharding import PartitionSpec as P


MESH = pl.DeviceIdType.MESH


def normalise(tokens, norm_gain):
    values = tokens.astype(jnp.float32)
    scale = lax.rsqrt(jnp.mean(values * values, axis=1, keepdims=True) + 1e-06)
    return (values * scale * norm_gain[None, :]).astype(jnp.bfloat16)


def activate(gate, upper):
    gate = jnp.minimum(gate, 7.0)
    upper = jnp.clip(upper, -7.0, 7.0)
    return (upper + 1.0) * (gate * jax.nn.sigmoid(1.702 * gate))


def routed(tokens, norm_gain, expert_ids, route_weights, gate_weight, up_weight, down_weight):
    tok_dev, width = tokens.shape
    top = expert_ids.shape[1]
    n_ep = lax.axis_size("ep")
    n_tp = lax.axis_size("tp")
    exp_dev = gate_weight.shape[0]
    experts = exp_dev * n_ep
    capacity = 2 * tok_dev * top // experts
    quarter = width // n_tp
    normed = normalise(tokens, norm_gain)
    flat = expert_ids.reshape(-1)
    count = flat.shape[0]
    onehot = (flat[:, None] == jnp.arange(experts, dtype=jnp.int32)[None, :]).astype(jnp.int32)
    before = jnp.cumsum(onehot, axis=0) - onehot
    slot = jnp.sum(before * onehot, axis=1)
    position = flat * capacity + slot
    source_tok = jnp.arange(count, dtype=jnp.int32) // top
    buffer_tok = jnp.zeros((experts * capacity,), jnp.int32).at[position].set(source_tok)
    buffer_live = jnp.zeros((experts * capacity,), jnp.int32).at[position].set(1)
    columns = lax.dynamic_slice_in_dim(normed, lax.axis_index("tp") * quarter, quarter, 1)
    outgoing = jnp.where(buffer_live[:, None] > 0, columns[buffer_tok], jnp.zeros((), jnp.bfloat16))
    outgoing = outgoing.reshape(n_ep, exp_dev, capacity, quarter)
    received = lax.all_gather(
        lax.all_to_all(outgoing, "ep", split_axis=0, concat_axis=0, tiled=True),
        "tp",
        axis=3,
        tiled=True,
    )
    gate = jnp.einsum("sxcd,xdf->sxcf", received, gate_weight, preferred_element_type=jnp.float32)
    upper = jnp.einsum("sxcd,xdf->sxcf", received, up_weight, preferred_element_type=jnp.float32)
    hidden = activate(gate, upper).astype(jnp.bfloat16)
    partial_value = jnp.einsum(
        "sxcf,xfd->sxcd", hidden, down_weight, preferred_element_type=jnp.float32
    )
    rounded = partial_value.astype(jnp.bfloat16)
    summed = lax.psum_scatter(rounded, "tp", scatter_dimension=3, tiled=True)
    returned = lax.all_to_all(summed, "ep", split_axis=0, concat_axis=0, tiled=True)
    returned = returned.reshape(experts * capacity, quarter)
    picked = returned[position].reshape(tok_dev, top, quarter)
    mixed = jnp.sum(route_weights[:, :, None] * picked.astype(jnp.float32), axis=1)
    return mixed.astype(jnp.bfloat16)


def kernel(
    n_ep, tokens_ref, gain_ref, route_ref, gate_hbm, up_hbm, down_hbm, out_ref,
    gath, gtab, route_buf, gate_w, up_w, down_w, hidden, part, dbuf, ya, xa, xb, yb, own, zin,
    w_sem, sz, rz, sx, rx, sy, ry, sd, rd,
    s_d, r_d, s_ya, r_ya, s_xb, r_xb, s_xa, r_xa, s_yb, r_yb, s_z, r_z,
):
    ep, tp = lax.axis_index("ep"), lax.axis_index("tp")
    z, x, y, c = ep // 2, ep % 2, tp // 2, tp % 2
    nz = n_ep // 2
    width = tokens_ref.shape[1]
    quarter = width // 4
    eighth = quarter // 2
    common = width // 8
    special = (width - 2 * common) // 4
    above = {"ep": lax.rem(ep + 2, n_ep), "tp": tp}
    below = {"ep": lax.rem(ep + n_ep - 2, n_ep), "tp": tp}
    xdev = {"ep": 2 * z + 1 - x, "tp": tp}
    ydev = {"ep": ep, "tp": 2 * (1 - y) + c}
    ddev = {"ep": ep, "tp": 2 * y + 1 - c}

    weight_copies = [
        pltpu.make_async_copy(gate_hbm.at[0], gate_w, w_sem.at[0]),
        pltpu.make_async_copy(up_hbm.at[0], up_w, w_sem.at[1]),
        pltpu.make_async_copy(down_hbm.at[0], down_w, w_sem.at[2]),
    ]
    for item in weight_copies:
        item.start()

    barrier = pltpu.get_barrier_semaphore()

    def greet(device):
        pl.semaphore_signal(barrier, inc=1, device_id=device, device_id_type=MESH)

    for device in (xdev, ydev, ddev):
        greet(device)

    def peer(k):
        return {"ep": lax.rem(ep + 2 * k, n_ep), "tp": tp}

    for k in range(1, nz):
        greet(peer(k))

    tile = 32

    def norm_step(i, carry):
        rows = pl.ds(pl.multiple_of(i * tile, tile), tile)
        values = tokens_ref[rows, :].astype(jnp.float32)
        scale = lax.rsqrt(jnp.mean(values * values, axis=1, keepdims=True) + 1e-06)
        gath[ep, rows, :] = (values * scale * gain_ref[...]).astype(jnp.bfloat16)
        return carry

    lax.fori_loop(0, tokens_ref.shape[0] // tile, norm_step, 0)
    gtab[ep] = route_ref[...]
    pl.semaphore_wait(barrier, 2 + nz)

    def cols(k, yy, cc):
        if k == 0:
            return pl.ds(pl.multiple_of(cc * common, 128), common)
        return pl.ds(pl.multiple_of(2 * common + (2 * yy + cc) * special, 128), special)

    def move(block, k, yy, cc, device, send, recv):
        ref = gtab.at[block] if k == 2 else gath.at[block, :, cols(k, yy, cc)]
        return pltpu.make_async_remote_copy(
            src_ref=ref, dst_ref=ref, send_sem=send, recv_sem=recv,
            device_id=device, device_id_type=MESH,
        )

    def go_z(block, k, direction):
        device = above if direction == 0 else below
        return move(block, k, y, c, device, sz.at[direction, k, block], rz.at[k, block])

    def go_x(block, k):
        return move(block, k, y, c, xdev, sx.at[k, block], rx.at[k, block])

    def go_y(block, yy):
        return move(block, 1, yy, c, ydev, sy.at[block], ry.at[block])

    def go_d(block, kind, cc):
        k, yy = (0, y) if kind == 0 else (1, y if kind == 1 else 1 - y)
        return move(block, k, yy, cc, ddev, sd.at[kind, block], rd.at[kind, block])

    for k in (1, 2, 0):
        @pl.when(z < nz - 1)
        def _():
            go_z(ep, k, 0).start()

        @pl.when(z > 0)
        def _():
            go_z(ep, k, 1).start()

        go_x(ep, k).start()

    def from_z(block, direction):
        for k in (1, 2, 0):
            go_z(block, k, direction).wait_recv()

            @pl.when(z < nz - 1 if direction == 0 else z > 0)
            def _():
                go_z(block, k, direction).start()

            go_x(block, k).start()
            if k == 1:
                go_y(block, y).start()
            if k < 2:
                go_d(block, k, c).start()

    def from_x(block):
        for k in (1, 2, 0):
            go_x(block, k).wait_recv()
            if k == 1:
                go_y(block, y).start()
            if k < 2:
                go_d(block, k, c).start()

    def from_y(block):
        go_y(block, 1 - y).wait_recv()
        go_d(block, 2, c).start()

    def at_distance(s, action):
        @pl.when(z - s >= 0)
        def _():
            action(z - s, 0)

        @pl.when(z + s <= nz - 1)
        def _():
            action(z + s, 1)

    for s in range(1, nz):
        at_distance(s, lambda row, way: from_z(2 * row + x, way))
        if s == 1:
            from_x(2 * z + 1 - x)
        else:
            at_distance(s - 1, lambda row, way: from_x(2 * row + 1 - x))
    at_distance(nz - 1, lambda row, way: from_x(2 * row + 1 - x))

    def others(action):
        action(2 * z + 1 - x)
        for s in range(1, nz):
            at_distance(s, lambda row, way: action(2 * row + x))
            at_distance(s, lambda row, way: action(2 * row + 1 - x))

    def arrived(block):
        for kind in (0, 1, 2):
            go_d(block, kind, 1 - c).wait_recv()

    def span(start, size):
        return pl.ds(pl.multiple_of(start, 128), size)

    def send(src, dst, send_sem, recv_sem, device):
        return pltpu.make_async_remote_copy(
            src_ref=src, dst_ref=dst, send_sem=send_sem, recv_sem=recv_sem,
            device_id=device, device_id_type=MESH,
        )

    pieces = 2
    rows = tokens_ref.shape[0] // pieces

    def half(u):
        return pl.ds(pl.multiple_of((u % pieces) * rows, 16), rows)

    def half_lane(u):
        return pl.ds(pl.multiple_of((u % pieces) * rows, 128), rows)

    def d_copy(u, yq, cc):
        r = u // pieces
        return send(
            part.at[pl.ds(2 * r, 2), half(u), span((2 * yq + cc) * quarter, quarter)],
            dbuf.at[pl.ds(2 * r, 2), half(u), span(yq * quarter, quarter)],
            s_d.at[u, yq], r_d.at[u, yq], ddev,
        )

    def ya_copy(u):
        r = u // pieces
        return send(
            dbuf.at[pl.ds(2 * r, 2), half(u), span((1 - y) * quarter, eighth)],
            ya.at[pl.ds(2 * r, 2), half(u)], s_ya.at[u], r_ya.at[u], ydev,
        )

    def xb_copy(u, yq):
        r = u // pieces
        return send(
            dbuf.at[2 * r + 1 - x, half(u), span(yq * quarter + eighth, eighth)],
            xb.at[r, half(u), span(yq * eighth, eighth)],
            s_xb.at[u, yq], r_xb.at[u, yq], xdev,
        )

    def xa_copy(u):
        r = u // pieces
        return send(
            ya.at[2 * r + 1 - x, half(u)], xa.at[r, half(u)], s_xa.at[u], r_xa.at[u], xdev
        )

    def yb_copy(u):
        r = u // pieces
        return send(
            xb.at[r, half(u), span((1 - y) * eighth, eighth)],
            yb.at[r, half(u)], s_yb.at[u], r_yb.at[u], ydev,
        )

    def z_copy(u, row):
        p = u % pieces
        return send(
            own.at[row, half(u)], zin.at[z, half(u)], s_z.at[u], r_z.at[z, p],
            {"ep": 2 * row + x, "tp": tp},
        )

    def z_wait(origin, p):
        return send(
            own.at[origin, half(p)], zin.at[origin, half(p)], s_z.at[p], r_z.at[origin, p],
            {"ep": 2 * origin + x, "tp": tp},
        )

    def add(a, b):
        return (a.astype(jnp.float32) + b.astype(jnp.float32)).astype(jnp.bfloat16)

    ff = gate_w.shape[1]
    fstep = min(256, ff)

    def compute(u):
        r = u // pieces
        lhs_of = lambda: gath[pl.ds(2 * r, 2), half(u)].reshape(2 * rows, width)
        for j in (0, 1):
            flipped = jnp.transpose(gtab[2 * r + j, :, half_lane(u)])
            lane = lax.broadcasted_iota(jnp.int32, flipped.shape, 1)
            column = jnp.sum(jnp.where(lane == ep, flipped, 0.0), axis=1, keepdims=True)
            route_buf[j * rows:(j + 1) * rows, :] = jnp.broadcast_to(column, (rows, 128))
        route = jnp.concatenate([route_buf[...]] * (fstep // 128), axis=1)

        def ff_step(j, carry):
            at = span(j * fstep, fstep)
            lhs = lhs_of()
            gate = jnp.dot(lhs, gate_w[:, at], preferred_element_type=jnp.float32)
            upper = jnp.dot(lhs, up_w[:, at], preferred_element_type=jnp.float32)
            value = activate(gate, upper)
            hidden[:, at] = jnp.where(route > 0, route * value, 0.0).astype(jnp.bfloat16)
            return carry

        lax.fori_loop(0, ff // fstep, ff_step, 0)

        def down_step(j, carry):
            yq = j % 2
            cc = jnp.where(j < 2, 1 - c, c)
            at = span((2 * yq + cc) * quarter, quarter)
            value = jnp.dot(hidden[...], down_w[:, at], preferred_element_type=jnp.float32)
            part[pl.ds(2 * r, 2), half(u), at] = value.astype(jnp.bfloat16).reshape(2, rows, quarter)

            @pl.when(j < 2)
            def _():
                d_copy(u, yq, 1 - c).start()

            return carry

        lax.fori_loop(0, 4, down_step, 0)

    def stage_a(u):
        r = u // pieces
        for yq in (0, 1):
            d_copy(u, yq, 1 - c).wait_recv()
            mine = part[pl.ds(2 * r, 2), half(u), span((2 * yq + c) * quarter, quarter)]
            at = span(yq * quarter, quarter)
            dbuf[pl.ds(2 * r, 2), half(u), at] = add(mine, dbuf[pl.ds(2 * r, 2), half(u), at])
        ya_copy(u).start()
        for yq in (0, 1):
            xb_copy(u, yq).start()

    def stage_b(u):
        r = u // pieces
        ya_copy(u).wait_recv()
        ya[pl.ds(2 * r, 2), half(u)] = add(
            dbuf[pl.ds(2 * r, 2), half(u), span(y * quarter, eighth)],
            ya[pl.ds(2 * r, 2), half(u)],
        )
        xa_copy(u).start()
        for yq in (0, 1):
            xb_copy(u, yq).wait_recv()
            at = span(yq * eighth, eighth)
            mine = dbuf[2 * r + x, half(u), span(yq * quarter + eighth, eighth)]
            xb[r, half(u), at] = add(mine, xb[r, half(u), at])
        yb_copy(u).start()

    def stage_c(u):
        r = u // pieces
        xa_copy(u).wait_recv()
        own[r, half(u), 0:eighth] = add(ya[2 * r + x, half(u)], xa[r, half(u)])
        yb_copy(u).wait_recv()
        own[r, half(u), eighth:quarter] = add(
            xb[r, half(u), span(y * eighth, eighth)], yb[r, half(u)]
        )

    def stage_d(u):
        r = u // pieces

        @pl.when(z != r)
        def _():
            z_copy(u, r).start()

    last_first = [nz - 1 - i // 2 if i % 2 == 0 else i // 2 for i in range(nz)]
    order = [[k] + [r for r in last_first if r != k] for k in range(nz)]
    units = nz * pieces

    def unit_of(i):
        row = z
        for k in range(nz):
            for j in range(1, nz):
                row = jnp.where((z == k) & (i // pieces == j), order[k][j], row)
        return row * pieces + i % pieces

    def step(i, carry):
        @pl.when(i == pieces)
        def _():
            for s in range(1, nz):
                at_distance(s, lambda row, way: from_y(2 * row + x))
                at_distance(s, lambda row, way: from_y(2 * row + 1 - x))
            for s in range(1, nz):
                at_distance(s, lambda row, way: arrived(2 * row + x))
                at_distance(s, lambda row, way: arrived(2 * row + 1 - x))

        @pl.when(i < units)
        def _():
            compute(unit_of(i))
            stage_a(unit_of(i))

        @pl.when((i >= 1) & (i < units + 1))
        def _():
            stage_b(unit_of(i - 1))

        @pl.when((i >= 2) & (i < units + 2))
        def _():
            stage_c(unit_of(i - 2))
            stage_d(unit_of(i - 2))

        return carry

    from_y(2 * z + 1 - x)
    arrived(2 * z + 1 - x)
    for item in weight_copies:
        item.wait()
    lax.fori_loop(0, units + 2, step, 0)

    for p in range(pieces):
        for k in range(1, nz):
            z_wait(lax.rem(z + k, nz), p).wait_recv()
        total = own[z, half(p)].astype(jnp.float32)
        for k in range(1, nz):
            total = total + zin[lax.rem(z + k, nz), half(p)].astype(jnp.float32)
        out_ref[half(p), :] = total.astype(jnp.bfloat16)

    def sent(block, direction):
        for k in (0, 1, 2):
            @pl.when(z < nz - 1 if direction == 0 else z > 0)
            def _():
                go_z(block, k, direction).wait_send()

            go_x(block, k).wait_send()

    for k in (0, 1, 2):
        @pl.when(z < nz - 1)
        def _():
            go_z(ep, k, 0).wait_send()

        @pl.when(z > 0)
        def _():
            go_z(ep, k, 1).wait_send()

        go_x(ep, k).wait_send()
    for s in range(1, nz):
        at_distance(s, lambda row, way: sent(2 * row + x, way))

    def passed(block):
        go_y(block, y).wait_send()
        for kind in (0, 1, 2):
            go_d(block, kind, c).wait_send()

    others(passed)

    def finish(u, carry):
        for yq in (0, 1):
            d_copy(u, yq, 1 - c).wait_send()
            xb_copy(u, yq).wait_send()
        ya_copy(u).wait_send()
        xa_copy(u).wait_send()
        yb_copy(u).wait_send()

        @pl.when(z != u // pieces)
        def _():
            z_copy(u, u // pieces).wait_send()

        return carry

    lax.fori_loop(0, units, finish, 0)


def dense(tokens, norm_gain, expert_ids, route_weights, gate_weight, up_weight, down_weight):
    rows, width = tokens.shape
    n_ep = lax.axis_size("ep")
    nz = n_ep // 2
    nu = nz * 2
    ff = gate_weight.shape[2]
    quarter = width // lax.axis_size("tp")
    eighth = quarter // 2
    onehot = expert_ids[:, :, None] == jnp.arange(n_ep, dtype=jnp.int32)[None, None, :]
    table = jnp.sum(jnp.where(onehot, route_weights[:, :, None], 0.0), axis=1)
    vmem = pl.BlockSpec(memory_space=pltpu.VMEM)
    hbm = pl.BlockSpec(memory_space=pl.ANY)
    bf16 = jnp.bfloat16
    dma = pltpu.SemaphoreType.DMA
    return pl.pallas_call(
        functools.partial(kernel, n_ep),
        out_shape=jax.ShapeDtypeStruct((rows, quarter), bf16),
        in_specs=[vmem, vmem, vmem, hbm, hbm, hbm],
        out_specs=vmem,
        scratch_shapes=[
            pltpu.VMEM((n_ep, rows, width), bf16),
            pltpu.VMEM((n_ep, n_ep, rows), jnp.float32),
            pltpu.VMEM((2 * rows // 2, 128), jnp.float32),
            pltpu.VMEM((width, ff), bf16),
            pltpu.VMEM((width, ff), bf16),
            pltpu.VMEM((ff, width), bf16),
            pltpu.VMEM((2 * rows // 2, ff), bf16),
            pltpu.VMEM((n_ep, rows, width), bf16),
            pltpu.VMEM((n_ep, rows, 2 * quarter), bf16),
            pltpu.VMEM((n_ep, rows, eighth), bf16),
            pltpu.VMEM((nz, rows, eighth), bf16),
            pltpu.VMEM((nz, rows, 2 * eighth), bf16),
            pltpu.VMEM((nz, rows, eighth), bf16),
            pltpu.VMEM((nz, rows, quarter), bf16),
            pltpu.VMEM((nz, rows, quarter), bf16),
            dma((3,)),
            dma((2, 3, n_ep)), dma((3, n_ep)),
            dma((3, n_ep)), dma((3, n_ep)),
            dma((n_ep,)), dma((n_ep,)),
            dma((3, n_ep)), dma((3, n_ep)),
            dma((nu, 2)), dma((nu, 2)),
            dma((nu,)), dma((nu,)),
            dma((nu, 2)), dma((nu, 2)),
            dma((nu,)), dma((nu,)),
            dma((nu,)), dma((nu,)),
            dma((nu,)), dma((nz, nu // nz)),
        ],
        compiler_params=pltpu.CompilerParams(
            collective_id=0, has_side_effects=True, vmem_limit_bytes=60 * 1024 * 1024
        ),
    )(tokens, norm_gain[None, :], table.T, gate_weight, up_weight, down_weight)


def per_device(tokens, norm_gain, expert_ids, route_weights, gate_weight, up_weight, down_weight):
    tok_dev, top = expert_ids.shape
    experts = gate_weight.shape[0] * lax.axis_size("ep")
    whole = gate_weight.shape[0] == 1 and 2 * tok_dev * top // experts >= tok_dev
    whole = whole and lax.axis_size("tp") == 4 and lax.axis_size("ep") % 2 == 0
    form = dense if whole and tokens.shape[1] % 2048 == 0 else routed
    return form(
        tokens, norm_gain, expert_ids, route_weights, gate_weight, up_weight, down_weight
    )


def solution(mesh):
    in_specs = (
        P("ep", None),
        P(),
        P("ep", None),
        P("ep", None),
        P("ep", None, "tp"),
        P("ep", None, "tp"),
        P("ep", "tp", None),
    )
    return jax.shard_map(
        per_device, mesh=mesh, in_specs=in_specs, out_specs=P("ep", "tp"), check_vma=False
    )
```
